32 devices in a mesh: sp: 16 (over z, y, x), tp: 2 (over core).
Axes of the slice: x: 2, y: 2, z: 4, core: 2. Of those that a mesh axis runs over, the one named last changes fastest.
Arguments:
- hidden_in: bfloat16 [8192, 2048], P('sp'), may hold values from -64 to 64
- pre_gain: float32 [2048], replicated, may hold values from 0.1 to 1.9
- query_proj: bfloat16 [2048, 2048], P(None, 'tp'), may hold values from -2 to 2
- key_proj: bfloat16 [2048, 2048], P('sp', 'tp'), may hold values from -2 to 2
- value_proj: bfloat16 [2048, 2048], P('sp', 'tp'), may hold values from -0.125 to 0.125
- out_proj: bfloat16 [2048, 2048], P('tp'), may hold values from -0.125 to 0.125
- post_gain: float32 [2048], replicated, may hold values from 0.1 to 1.9
Outputs:
- layer_out: bfloat16 [8192, 2048], P(('sp', 'tp'))
- log_weight: float32 [32, 8192], P('tp', 'sp')
The draws below stay inside these ranges and needn't reach their ends.
All inputs are finite; a program needn't handle non-finite values.
Results may differ from the reference program's by a relative error of at most 0.018.
The reference program's roundings to bfloat16 on the way count: a program that leaves them out, or rounds other values in their place, can miss the bound.
Values may be sent and summed in bfloat16 or wider, within the bound.
No kernel may reach another device: no remote copies, remote signals or barrier semaphores. Data moves between devices by JAX's collectives and lax.ppermute only.
A program may use at most 128 MiB of HBM per device.

```python
import jax
import jax.numpy as jnp
from jax import lax

D = 2048
HEADS = 32
HEAD_DIM = 64
SPAN = 128
TOKENS = 8192
N_TP = 2


def draw_hidden_in(key, part):
    noise_part = jax.random.normal(jax.random.fold_in(key, 3), (TOKENS, D), jnp.float32)
    return jnp.clip(noise_part, -64.0, 64.0).astype(jnp.bfloat16)


def shared_pair(key):
    fan_scale = D ** (-0.5)
    query_part = jax.random.normal(jax.random.fold_in(key, 22), (D, HEADS * HEAD_DIM), jnp.float32) * fan_scale
    key_part = jax.random.normal(jax.random.fold_in(key, 23), (D, HEADS * HEAD_DIM), jnp.float32) * fan_scale
    return (jnp.clip(query_part, -2.0, 2.0), jnp.clip(key_part, -2.0, 2.0))


def draw_query_proj(key, part):
    return shared_pair(key)[0].astype(jnp.bfloat16)


def draw_key_proj(key, part):
    return shared_pair(key)[1].astype(jnp.bfloat16)


def steps_of(key, dims, split, least, high):
    factor_of = 1.0
    for dim, parts in split:
        steps = jax.random.uniform(jax.random.fold_in(jax.random.fold_in(key, 6), dim), (parts,), jnp.float32, least / len(split), high / len(split))
        factor_of = factor_of * jnp.repeat(jnp.exp(steps), dims[dim] // parts).reshape((-1,) + (1,) * (len(dims) - 1 - dim))
    return factor_of


def noise(key, shape, deviation, most, shards=(), held_as=jnp.bfloat16):
    values = jax.random.normal(key, shape, jnp.float32) * deviation
    if len(shards) > 0:
        values = steps_of(key, shape, shards, -0.22, 0.18) * values
    return jnp.clip(values, min=-most, max=most).astype(held_as)


def setup_inputs(seed: int = 0) -> dict:
    splits = jax.random.split(jax.random.key(seed), 8)
    return {
        "hidden_in": draw_hidden_in(jax.random.fold_in(splits[7], 71), 0),
        "pre_gain": jnp.clip(1.0 + 0.18 * jax.random.normal(splits[1], (D,), jnp.float32), 0.1, 1.9),
        "query_proj": draw_query_proj(jax.random.fold_in(splits[7], 71), 0),
        "key_proj": draw_key_proj(jax.random.fold_in(splits[7], 71), 0),
        "value_proj": noise(splits[4], (D, HEADS * HEAD_DIM), D ** -0.5, 0.125, ((0, 16), (1, 2))),
        "out_proj": noise(splits[5], (HEADS * HEAD_DIM, D), (HEADS * HEAD_DIM) ** -0.5, 0.125, ((0, 2),)),
        "post_gain": jnp.clip(1.0 + 0.18 * jax.random.normal(splits[6], (D,), jnp.float32), 0.1, 1.9),
    }


EPS = 1e-06
ROPE_BASE = 10000.0
DILATIONS = (1, 4, 16)

def rotate(vectors, positions):
    half_dim = vectors.shape[-1] // 2
    frequency = ROPE_BASE ** (-(jnp.arange(half_dim, dtype=jnp.float32) * 2.0 / vectors.shape[-1]))
    angles = positions[:, None] * frequency[None, :]
    cos_part = jnp.cos(angles)[:, None, :]
    sin_part = jnp.sin(angles)[:, None, :]
    front_half = vectors[..., :half_dim]
    back_half = vectors[..., half_dim:]
    return jnp.concatenate([front_half * cos_part - back_half * sin_part, back_half * cos_part + front_half * sin_part], axis=-1)

def rms_scale(matrix, gain):
    return matrix * lax.rsqrt(lax.optimization_barrier(jnp.mean(matrix * matrix, axis=-1, keepdims=True)) + EPS) * gain

def residue_attention(queries, key_rows, values, dilation):
    seq_len, head_count, head_depth = queries.shape
    blocks = seq_len // (dilation * SPAN)
    block_shape = (blocks, SPAN, dilation, head_count, head_depth)
    query_blocks = queries.reshape(block_shape).astype(jnp.float32)
    key_blocks = key_rows.reshape(block_shape).astype(jnp.float32)
    value_blocks = values.reshape(block_shape).astype(jnp.float32)
    zero_block = jnp.zeros((1,) + block_shape[1:], jnp.float32)
    key_pairs = jnp.concatenate([jnp.concatenate([zero_block, key_blocks[:-1]], axis=0), key_blocks], axis=1)
    value_pairs = jnp.concatenate([jnp.concatenate([zero_block, value_blocks[:-1]], axis=0), value_blocks], axis=1)
    scores = jnp.einsum('bqrhe,bkrhe->brhqk', query_blocks, key_pairs) * head_depth ** (-0.5)
    query_idx = jnp.arange(SPAN, dtype=jnp.int32)[:, None]
    key_idx = jnp.arange(2 * SPAN, dtype=jnp.int32)[None, :]
    distance = query_idx + SPAN - key_idx
    in_band = (distance >= 0) & (distance <= SPAN)
    key_pos = (jnp.arange(blocks, dtype=jnp.int32)[:, None, None, None, None] * SPAN + jnp.arange(2 * SPAN, dtype=jnp.int32)[None, None, None, None, :] - SPAN) * dilation + jnp.arange(dilation, dtype=jnp.int32)[None, :, None, None, None]
    valid = in_band[None, None, None] & (key_pos >= 0)
    scores = jnp.where(valid, scores, -jnp.inf)
    row_max = lax.optimization_barrier(jnp.max(scores, axis=-1, keepdims=True))
    exp_scores = jnp.exp(scores - row_max)
    denominator = lax.optimization_barrier(jnp.sum(exp_scores, axis=-1, keepdims=True))
    levels = (row_max + jnp.log(denominator))[..., 0]
    shares = lax.optimization_barrier((exp_scores / denominator).astype(jnp.bfloat16))
    outcome = jnp.einsum('brhqk,bkrhe->bqrhe', shares.astype(jnp.float32), value_pairs)
    outcome = outcome.reshape(seq_len, head_count, head_depth)
    levels = levels.transpose(2, 0, 3, 1).reshape(head_count, seq_len)
    return (outcome, levels)

def blend(group_outs, group_levels):
    levels = jnp.stack(group_levels)
    row_max = lax.optimization_barrier(jnp.max(levels, axis=0))
    log_weight = row_max + jnp.log(lax.optimization_barrier(jnp.sum(jnp.exp(levels - row_max[None]), axis=0)))
    shares = jnp.exp(levels - log_weight[None])
    blended = lax.optimization_barrier(jnp.sum(shares.transpose(0, 2, 1)[..., None] * jnp.stack(group_outs), axis=0))
    return (blended, log_weight)

def reference(hidden_in, pre_gain, query_proj, key_proj, value_proj, out_proj, post_gain):
    normed = rms_scale(hidden_in.astype(jnp.float32), pre_gain).astype(jnp.bfloat16)
    positions = jnp.arange(TOKENS, dtype=jnp.int32).astype(jnp.float32)
    group_width = HEADS // N_TP * HEAD_DIM

    def split_cols(matrix):
        return matrix.reshape(D, N_TP, group_width).transpose(1, 0, 2)

    def one_group(summed, weights):
        w_query, w_key, w_value, w_out = weights
        queries = rotate(jnp.dot(normed, w_query, preferred_element_type=jnp.float32).reshape(TOKENS, -1, HEAD_DIM), positions).astype(jnp.bfloat16)
        key_rows = rotate(jnp.dot(normed, w_key, preferred_element_type=jnp.float32).reshape(TOKENS, -1, HEAD_DIM), positions).astype(jnp.bfloat16)
        values = jnp.dot(normed, w_value, preferred_element_type=jnp.float32).astype(jnp.bfloat16).reshape(TOKENS, -1, HEAD_DIM)
        group_outs = []
        group_levels = []
        for dilation in DILATIONS:
            outcome, levels = residue_attention(queries, key_rows, values, dilation)
            group_outs.append(outcome)
            group_levels.append(levels)
        blended, log_weight = blend(group_outs, group_levels)
        attended = blended.astype(jnp.bfloat16).reshape(TOKENS, group_width)
        partial_value = lax.optimization_barrier(jnp.dot(attended, w_out, preferred_element_type=jnp.float32).astype(jnp.bfloat16))
        return (summed + partial_value.astype(jnp.float32), log_weight)
    summed, log_weight = lax.scan(one_group, jnp.zeros((TOKENS, D), jnp.float32), (split_cols(query_proj), split_cols(key_proj), split_cols(value_proj), out_proj.reshape(N_TP, group_width, D)))
    layer_out = rms_scale(summed, post_gain).astype(jnp.bfloat16)
    return (layer_out, log_weight.reshape(HEADS, TOKENS))
```

```python
import functools

import jax
import jax.numpy as jnp
from jax import lax
from jax.experimental import pallas as pl
from jax.experimental.pallas import tpu as pltpu
from jax.sharding import PartitionSpec as P

HEAD_DIM = 64
SPAN = 128
EPS = 1e-06
ROPE_BASE = 10000.0
DILATIONS = (1, 4, 16)
STEP = max(DILATIONS)
SUB = SPAN // STEP
NEG = -1e30
LANES = 128
F32 = jnp.float32
BF16 = jnp.bfloat16
SMEM = pl.BlockSpec(memory_space=pltpu.SMEM)
MIB = 1 << 20


def sds(shape, dtype):
    return jax.ShapeDtypeStruct(shape, dtype)


def lanes_of(width):
    return min(LANES, width)


def norm_body(hidden_ref, gain_ref, out_ref, scratch):
    rows = hidden_ref[...].astype(F32)
    mean = jnp.mean(rows * rows, axis=-1, keepdims=True)
    rows = rows * lax.rsqrt(mean + EPS) * gain_ref[...]
    for c in range(scratch.shape[0]):
        cols = slice(c * LANES, (c + 1) * LANES)
        scratch[c] = rows[:, cols]
        for r in range(0, STEP, 2):
            pair = [scratch[c, pl.ds(r + i, SUB, stride=STEP), :] for i in range(2)]
            out_ref[r * SUB : (r + 2) * SUB, cols] = jnp.concatenate(pair, axis=0).astype(BF16)


def norm_rows(hidden, gain):
    rows, width = hidden.shape
    return pl.pallas_call(
        norm_body,
        grid=(rows // SPAN,),
        in_specs=[
            pl.BlockSpec((SPAN, width), lambda i: (i, 0)),
            pl.BlockSpec((1, width), lambda i: (0, 0)),
        ],
        out_specs=pl.BlockSpec((SPAN, width), lambda i: (i, 0)),
        out_shape=sds((rows, width), BF16),
        scratch_shapes=[pltpu.VMEM((width // LANES, SPAN, LANES), F32)],
        compiler_params=pltpu.CompilerParams(vmem_limit_bytes=12 * MIB),
        name="norm_rows",
    )(hidden, gain.reshape(1, width))


def gather_body(idx, *refs):
    out_ref = refs[-1]
    for j, ref in enumerate(refs[:-1]):
        out_ref[idx[0] ^ j] = ref[...]


def gather_pieces(idx, pieces):
    return pl.pallas_call(
        gather_body,
        in_specs=[SMEM] + [pl.BlockSpec(memory_space=pltpu.VMEM)] * len(pieces),
        out_shape=sds((len(pieces),) + pieces[0].shape, pieces[0].dtype),
        compiler_params=pltpu.CompilerParams(vmem_limit_bytes=8 * MIB),
        name="gather_pieces",
    )(idx, *pieces)


def swap_halves(part):
    width = part.shape[-1]
    half = HEAD_DIM // 2
    if width == HEAD_DIM:
        return jnp.concatenate([part[:, half:], part[:, :half]], axis=-1)
    lane = lax.broadcasted_iota(jnp.int32, part.shape, 1)
    front = (lane & (HEAD_DIM - 1)) < half
    return jnp.where(front, pltpu.roll(part, width - half, 1), pltpu.roll(part, half, 1))


def rotated(rows, cos, sin):
    width = cos.shape[-1]
    parts = []
    for lo in range(0, rows.shape[-1], width):
        part = rows[:, lo : lo + width]
        parts.append(part * cos + swap_halves(part) * sin)
    return parts[0] if len(parts) == 1 else jnp.concatenate(parts, axis=-1)


def project_body(plan, local_rows, planes, idx, *refs):
    chunks = refs[: len(plan)]
    refs = refs[len(plan) :]
    own, ups, downs = refs[0], refs[1:planes], refs[planes : 2 * planes - 1]
    wq, cos_ref, sin_ref, q1, qr, k1, v1, kvr, wkv, scratch = refs[2 * planes - 1 :]
    place, plane, part = idx[0], idx[1], idx[2]
    depth = own.shape[0]
    width = wq.shape[1]

    def put(which, ref):
        wkv[pl.ds(pl.multiple_of(which * depth, depth), depth), :] = ref[...]

    put(plane, own)
    for k in range(1, planes):
        pl.when(plane >= k)(functools.partial(put, plane - k, ups[k - 1]))
        pl.when(plane + k < planes)(functools.partial(put, plane + k, downs[k - 1]))
    scale = HEAD_DIM**-0.5
    for j in sorted({entry[0] for entry in plan}):
        base = pl.multiple_of((place ^ j) * local_rows, local_rows)
        base_r = pl.multiple_of((place ^ j) * (local_rows // STEP), local_rows // STEP)
        for name, flat, split in (("q", q1, qr), ("k", k1, kvr.at[0]), ("v", v1, kvr.at[1])):
            for (jj, k, size, off), chunk in zip(plan, chunks):
                if jj != j:
                    continue
                weight = wq[...] if name == "q" else None
                if name == "k":
                    weight = wkv[:, :width]
                if name == "v":
                    weight = wkv[:, width:]
                rows = chunk.shape[0]
                at = 0 if size is None else pl.multiple_of((part ^ k) * size + off, rows)
                for lo in range(0, rows, 256):
                    few = min(256, rows - lo)
                    out = jnp.dot(chunk[lo : lo + few, :], weight, preferred_element_type=F32)
                    if name != "v":
                        table = pl.ds(pl.multiple_of(base + at + lo, few), few)
                        out = rotated(out, cos_ref[table, :], sin_ref[table, :])
                    if name == "q":
                        out = out * scale
                    scratch[pl.ds(pl.multiple_of(at + lo, few), few), :] = out
            flat[pl.ds(base, local_rows), :] = scratch[...].astype(BF16)
            for r in range(STEP):
                slabs = [
                    scratch[b * SPAN + r * SUB : b * SPAN + (r + 1) * SUB, :]
                    for b in range(local_rows // SPAN)
                ]
                split[r, pl.ds(base_r, local_rows // STEP), :] = jnp.concatenate(slabs, axis=0).astype(BF16)


def project(idx, plan, chunks, weights, wq, tables, local_rows, total):
    own, ups, downs = weights
    width = wq.shape[1]
    flat = sds((total, width), BF16)
    split = sds((STEP, total // STEP, width), BF16)
    count = len(chunks) + 1 + len(ups) + len(downs) + 3
    return pl.pallas_call(
        functools.partial(project_body, plan, local_rows, len(ups) + 1),
        in_specs=[SMEM] + [pl.BlockSpec(memory_space=pltpu.VMEM)] * count,
        out_shape=(flat, split, flat, flat, sds((2,) + split.shape, BF16)),
        scratch_shapes=[
            pltpu.VMEM((wq.shape[0], 2 * width), BF16),
            pltpu.VMEM((local_rows, width), F32),
        ],
        compiler_params=pltpu.CompilerParams(vmem_limit_bytes=48 * MIB),
        name="project",
    )(idx, *chunks, own, *ups, *downs, wq, *tables)


def steps_of(index, members, count, start):
    return ((index & (count - 1)) + start) * members + (index >> (count.bit_length() - 1))


def band(query_steps, key_steps):
    gap = query_steps - key_steps
    return jnp.where((gap >= 0) & (gap <= SPAN), 0.0, NEG).astype(F32)


def band_of(members, count, start):
    shape = (SPAN, members * count)
    query = steps_of(lax.broadcasted_iota(jnp.int32, shape, 0), members, SPAN // members, 0)
    return band(query, steps_of(lax.broadcasted_iota(jnp.int32, shape, 1), members, count, start))


def attend(query, keys, values, mask):
    width = query.shape[1]
    heads = width // HEAD_DIM
    group = lanes_of(width)
    per_group = group // HEAD_DIM
    owner = lax.broadcasted_iota(jnp.int32, query.shape, 1) >> (HEAD_DIM.bit_length() - 1)
    zero = jnp.zeros_like(query)
    stacked = [jnp.where(owner == h, query, zero) for h in range(heads)] if heads > 1 else [query]
    scores = lax.dot_general(
        jnp.concatenate(stacked, axis=0) if heads > 1 else query,
        keys,
        (((1,), (1,)), ((), ())),
        preferred_element_type=F32,
    )
    lane = lax.broadcasted_iota(jnp.int32, (SPAN, group), 1) >> (HEAD_DIM.bit_length() - 1)
    ones = jnp.ones((keys.shape[0], group), BF16)
    tops, sums, outs = [], [], []
    for g in range(heads // per_group):
        maxima, exps = [], []
        for h in range(g * per_group, (g + 1) * per_group):
            part = scores[h * SPAN : (h + 1) * SPAN, :] + mask
            top = jnp.max(part, axis=-1, keepdims=True)
            exps.append(jnp.exp(part - top).astype(BF16))
            maxima.append(jnp.broadcast_to(top, (SPAN, group)))
        exps = jnp.concatenate(exps, axis=0) if per_group > 1 else exps[0]
        mine = values[:, g * group : (g + 1) * group]
        if group == LANES:
            both = jnp.dot(exps, jnp.concatenate([mine, ones], axis=1), preferred_element_type=F32)
            out, total = both[:, :group], both[:, group:]
        else:
            out = jnp.dot(exps, mine, preferred_element_type=F32)
            total = jnp.dot(exps, ones, preferred_element_type=F32)

        def pick(parts):
            chosen = parts[0]
            for i in range(1, per_group):
                chosen = jnp.where(lane == i, parts[i], chosen)
            return chosen

        tops.append(pick(maxima))
        sums.append(pick([total[i * SPAN : (i + 1) * SPAN] for i in range(per_group)]))
        outs.append(pick([out[i * SPAN : (i + 1) * SPAN] for i in range(per_group)]))
    return [jnp.concatenate(x, axis=1) if len(x) > 1 else x[0] for x in (tops, sums, outs)]


def merged(old, new):
    top = jnp.maximum(old[0], new[0])
    keep, add = jnp.exp(old[0] - top), jnp.exp(new[0] - top)
    return [top, old[1] * keep + new[1] * add, old[2] * keep + new[2] * add]


def slabs_of(refs, members, first, stride, block, count):
    width = refs[0].shape[-1]
    return [
        jnp.concatenate(
            [
                ref[pl.ds(block, count), first + stride * a].reshape(count * SUB, width)
                for a in range(members)
            ],
            axis=0,
        )
        for ref in refs
    ]


def put_slabs(refs, values, members, first, stride, block, count):
    width = refs[0].shape[-1]
    for ref, value in zip(refs, values):
        for a in range(members):
            rows = value[a * count * SUB : (a + 1) * count * SUB, :]
            ref[pl.ds(block, count), first + stride * a] = rows.reshape(count, SUB, width)


def class_rows(ref, members, first, stride, start, count):
    parts = [ref[first + stride * a, pl.ds(start, count), :] for a in range(members)]
    return parts[0] if members == 1 else jnp.concatenate(parts, axis=0)


def local_body(q1, qr, k1, v1, kvr, top_ref, sum_ref, out_ref, mask_ref, half_ref):
    total, width = q1.shape
    blocks = total // SPAN
    state = (top_ref, sum_ref, out_ref)
    own = band_of(STEP, SUB, 0)
    half_ref[...] = own
    mask_ref[:, :SPAN] = band_of(STEP, SUB, -SUB)
    mask_ref[:, SPAN:] = own

    def write(block, values):
        for ref, value in zip(state, values):
            ref[block] = value.reshape(STEP, SUB, width)

    write(0, attend(q1[:SPAN, :], k1[:SPAN, :], v1[:SPAN, :], half_ref[...]))

    def near(block, carry):
        rows = pl.ds(pl.multiple_of(block * SPAN, SPAN), SPAN)
        behind = pl.ds(pl.multiple_of((block - 1) * SPAN, SPAN), 2 * SPAN)
        write(block, attend(q1[rows, :], k1[behind, :], v1[behind, :], mask_ref[...]))
        return carry

    lax.fori_loop(1, blocks, near, 0)
    for dilation in DILATIONS[1:]:
        members = STEP // dilation
        count = SPAN // members
        each = count // SUB
        half_ref[...] = band_of(members, count, 0)
        mask_ref[...] = band_of(members, 2 * count, -count)
        sets = blocks // each

        def first(res, carry):
            where = (members, res, dilation, 0, count)
            new = attend(
                class_rows(qr, *where),
                class_rows(kvr.at[0], *where),
                class_rows(kvr.at[1], *where),
                half_ref[...],
            )
            at = (members, res, dilation, 0, each)
            put_slabs(state, merged(slabs_of(state, *at), new), *at)
            return carry

        lax.fori_loop(0, dilation, first, 0)
        if sets == 1:
            continue

        def later(step, carry):
            res = step // (sets - 1)
            block = step - res * (sets - 1) + 1
            start = pl.multiple_of(block * count, count)
            behind = pl.multiple_of((block - 1) * count, count)
            new = attend(
                class_rows(qr, members, res, dilation, start, count),
                class_rows(kvr.at[0], members, res, dilation, behind, 2 * count),
                class_rows(kvr.at[1], members, res, dilation, behind, 2 * count),
                mask_ref[...],
            )
            at = (members, res, dilation, block * each, each)
            put_slabs(state, merged(slabs_of(state, *at), new), *at)
            return carry

        lax.fori_loop(0, dilation * (sets - 1), later, 0)


def attend_local(q1, qr, k1, v1, kvr):
    total, width = q1.shape
    state = sds((total // SPAN, STEP, SUB, width), F32)
    return pl.pallas_call(
        local_body,
        in_specs=[pl.BlockSpec(memory_space=pltpu.VMEM)] * 5,
        out_shape=(state,) * 3,
        scratch_shapes=[pltpu.VMEM((SPAN, 2 * SPAN), F32), pltpu.VMEM((SPAN, SPAN), F32)],
        compiler_params=pltpu.CompilerParams(vmem_limit_bytes=32 * MIB),
        name="attend_local",
    )(q1, qr, k1, v1, kvr)


def halo_body(idx, q1, qr, halo, top_in, sum_in, out_in, att_ref, level_ref, top_ref, sum_ref, out_ref, half_ref, near_ref, turn, turn_level):
    total, width = q1.shape
    blocks = total // SPAN
    group = lanes_of(width)
    groups = width // group
    state = (top_ref, sum_ref, out_ref)
    given = (top_in, sum_in, out_in)
    for ref, source in zip(state, given):
        ref[...] = source[...]

    @pl.when(idx[1] > 0)
    def _():
        pair = 2 * SUB
        near_ref[...] = band_of(STEP, pair, -pair)
        last = total // STEP
        new = attend(
            q1[:SPAN, :],
            class_rows(halo.at[0], STEP, 0, 1, last - pair, pair),
            class_rows(halo.at[1], STEP, 0, 1, last - pair, pair),
            near_ref[...],
        )
        old = [ref[0].reshape(SPAN, width) for ref in state]
        for ref, value in zip(state, merged(old, new)):
            ref[0] = value.reshape(STEP, SUB, width)
        for dilation in DILATIONS[1:]:
            members = STEP // dilation
            count = SPAN // members
            each = count // SUB
            half_ref[...] = band_of(members, count, -count)

            def first(res, carry):
                where = (members, res, dilation, last - count, count)
                new = attend(
                    class_rows(qr, members, res, dilation, 0, count),
                    class_rows(halo.at[0], *where),
                    class_rows(halo.at[1], *where),
                    half_ref[...],
                )
                at = (members, res, dilation, 0, each)
                put_slabs(state, merged(slabs_of(state, *at), new), *at)
                return carry

            lax.fori_loop(0, dilation, first, 0)

    spread = att_ref.shape[1] // SPAN
    for block in range(blocks):
        top, denominator, out = [ref[block].reshape(SPAN, width) for ref in state]
        level = top + jnp.log(denominator)
        out = out / denominator
        for g in range(groups):
            turn[g, :, :group] = out[:, g * group : (g + 1) * group]
        chosen = level[:, :group]
        lane = lax.broadcasted_iota(jnp.int32, (SPAN, group), 1)
        for g in range(1, groups):
            chosen = jnp.where((lane & (HEAD_DIM - 1)) == g, level[:, g * group : (g + 1) * group], chosen)
        turn_level[:, :group] = chosen
        place, low = block // spread, (block % spread) * SPAN
        rows = []
        for m in range(SUB):
            here = slice(low + m * STEP, low + (m + 1) * STEP)
            for g in range(groups):
                spun = turn[g, pl.ds(m, STEP, stride=SUB), :]
                att_ref[place, here, g * group : (g + 1) * group] = spun[:, :group].astype(BF16)
            rows.append(turn_level[pl.ds(m, STEP, stride=SUB), :])
        flipped = jnp.concatenate(rows, axis=0).T
        for h in range(width // HEAD_DIM):
            source = (h % (group // HEAD_DIM)) * HEAD_DIM + h // (group // HEAD_DIM)
            level_ref[place, h : h + 1, low : low + SPAN] = flipped[source : source + 1, :]


def attend_halo(idx, q1, qr, halo, state, places):
    total, width = q1.shape
    local_rows = total // places
    group = lanes_of(width)
    full = pltpu.VMEM(state[0].shape, F32)
    return pl.pallas_call(
        halo_body,
        in_specs=[SMEM] + [pl.BlockSpec(memory_space=pltpu.VMEM)] * 6,
        out_shape=(
            sds((places, local_rows, width), BF16),
            sds((places, width // HEAD_DIM, local_rows), F32),
        ),
        scratch_shapes=[
            full,
            full,
            full,
            pltpu.VMEM((SPAN, SPAN), F32),
            pltpu.VMEM((SPAN, 2 * SPAN), F32),
            pltpu.VMEM((width // group, SPAN, LANES), F32),
            pltpu.VMEM((SPAN, LANES), F32),
        ],
        compiler_params=pltpu.CompilerParams(vmem_limit_bytes=40 * MIB),
        name="attend_halo",
    )(idx, q1, qr, halo, *state)


def out_body(idx, *refs):
    parts = refs[-1].shape[0]
    weight, out_ref = refs[-2], refs[-1]
    pieces = refs[:-2]
    rows, width = out_ref.shape[1], pieces[0].shape[1]
    for k in range(parts):
        at = pl.ds(pl.multiple_of((idx[2] ^ k) * rows, rows), rows)
        total = None
        for j, piece in enumerate(pieces):
            mine = weight[pl.ds(pl.multiple_of((idx[0] ^ j) * width, width), width), :]
            term = jnp.dot(piece[at, :], mine, preferred_element_type=F32)
            total = term if total is None else total + term
        out_ref[k] = total.astype(BF16)


def out_partials(idx, pieces, weight, parts):
    rows, width = pieces[0].shape
    depth, wide = weight.shape
    tile = min(512, wide)
    return pl.pallas_call(
        out_body,
        grid=(wide // tile,),
        in_specs=[SMEM]
        + [pl.BlockSpec((rows, width), lambda i: (0, 0))] * len(pieces)
        + [pl.BlockSpec((depth, tile), lambda i: (0, i))],
        out_specs=pl.BlockSpec((parts, rows // parts, tile), lambda i: (0, 0, i)),
        out_shape=sds((parts, rows // parts, wide), BF16),
        compiler_params=pltpu.CompilerParams(vmem_limit_bytes=16 * MIB),
        name="out_partials",
    )(idx, *pieces, weight)


def final_body(*refs):
    gain_ref, out_ref = refs[-2], refs[-1]
    summed = refs[0][...].astype(F32)
    for ref in refs[1:-2]:
        summed = summed + ref[...].astype(F32)
    mean = jnp.mean(summed * summed, axis=-1, keepdims=True)
    out_ref[...] = (summed * lax.rsqrt(mean + EPS) * gain_ref[...]).astype(BF16)


def final_norm(pieces, gain):
    rows, width = pieces[0].shape
    tile = min(128, rows)
    block = pl.BlockSpec((tile, width), lambda i: (i, 0))
    return pl.pallas_call(
        final_body,
        grid=(rows // tile,),
        in_specs=[block] * len(pieces) + [pl.BlockSpec((1, width), lambda i: (0, 0))],
        out_specs=block,
        out_shape=sds((rows, width), BF16),
        compiler_params=pltpu.CompilerParams(vmem_limit_bytes=16 * MIB),
        name="final_norm",
    )(*pieces, gain.reshape(1, width))


def body(hidden_in, pre_gain, query_proj, key_proj, value_proj, out_proj, post_gain):
    local_rows, model = hidden_in.shape
    devices, parts = lax.axis_size("sp"), lax.axis_size("tp")
    heads = query_proj.shape[1] // HEAD_DIM
    places = STEP * SPAN // local_rows
    if places < 1 or devices % places or heads % places or local_rows % SPAN:
        raise ValueError("unsupported split")
    planes = devices // places
    total = places * local_rows
    width = heads // places * HEAD_DIM
    index, part = lax.axis_index("sp"), lax.axis_index("tp")
    place, plane = index % places, index // places
    idx = jnp.stack([place, plane, part]).astype(jnp.int32)

    def across(value, j):
        return lax.ppermute(value, "sp", [(s, s ^ j) for s in range(devices)])

    def upward(value, sign=1):
        moves = [(s, s + sign * places) for s in range(devices)]
        return lax.ppermute(value, "sp", [m for m in moves if 0 <= m[1] < devices])

    def partner(value, k):
        return lax.ppermute(value, "tp", [(s, s ^ k) for s in range(parts)])

    def columns(j):
        at = (place ^ j) * width
        size = (key_proj.shape[0], width)
        return jnp.concatenate([lax.dynamic_slice(w, (0, at), size) for w in (key_proj, value_proj)], axis=1)

    pieces = [columns(0)] + [across(columns(j), j) for j in range(1, places)]
    own = gather_pieces(idx, pieces).reshape(places * key_proj.shape[0], 2 * width)
    ups, downs = [], []
    for k in range(1, planes):
        ups.append(upward(ups[-1] if ups else own, 1))
        downs.append(upward(downs[-1] if downs else own, -1))

    normed = norm_rows(hidden_in, pre_gain)
    size = local_rows // parts
    mine = lax.dynamic_slice(normed, (part * size, 0), (size, model))
    arrived = []
    if places == 4:
        one, two = across(mine, 1), across(mine, 2)
        half = size // 2
        arrived = [(1, 0, one), (2, 0, two), (3, 0, across(two[:half], 1)), (3, half, across(one[half:], 2))]
    else:
        arrived = [(j, 0, across(mine, j)) for j in range(1, places)]
    plan, chunks = [(0, 0, None, 0)], [normed]
    for j, off, rows in arrived:
        for k in range(parts):
            plan.append((j, k, size, off))
            chunks.append(rows if k == 0 else partner(rows, k))

    wide = lanes_of(width)
    token = jnp.arange(total, dtype=jnp.int32).reshape(total // SPAN, SUB, STEP).transpose(0, 2, 1).reshape(total)
    positions = (plane * total + token).astype(F32)
    lane = jnp.arange(wide, dtype=jnp.int32) % HEAD_DIM
    half_dim = HEAD_DIM // 2
    frequency = ROPE_BASE ** (-((lane % half_dim).astype(F32) * 2.0 / HEAD_DIM))
    angles = positions[:, None] * frequency[None, :]
    tables = (jnp.cos(angles), jnp.sin(angles) * jnp.where(lane < half_dim, -1.0, 1.0)[None, :])

    wq = lax.dynamic_slice(query_proj, (0, place * width), (model, width))
    q1, qr, k1, v1, kvr = project(idx, tuple(plan), chunks, (own, ups, downs), wq, tables, local_rows, total)
    halo = upward(kvr)
    state = attend_local(q1, qr, k1, v1, kvr)
    attended, levels = attend_halo(idx, q1, qr, halo, state, places)

    def swapped(value):
        slices = [lax.dynamic_index_in_dim(value, place ^ j, 0, keepdims=False) for j in range(places)]
        return [slices[0]] + [across(slices[j], j) for j in range(1, places)]

    partials = out_partials(idx, swapped(attended), out_proj, parts)
    log_weight = gather_pieces(idx, swapped(levels)).reshape(heads, local_rows)
    layer_out = final_norm([partials[0]] + [partner(partials[k], k) for k in range(1, parts)], post_gain)
    return (layer_out, log_weight)


def solution(mesh):
    placed = (P("sp", None), P(), P(None, "tp"), P("sp", "tp"), P("sp", "tp"), P("tp", None), P())
    return jax.shard_map(
        body,
        mesh=mesh,
        in_specs=placed,
        out_specs=(P(("sp", "tp"), None), P("tp", "sp")),
        check_vma=False,
    )
```
